32 devices in a mesh: kv: 16 (over z, y, x), tp: 2 (over core).
Axes of the slice: x: 2, y: 2, z: 4, core: 2. Of those that a mesh axis runs over, the one named last changes fastest.
Arguments:
- hidden_in: bfloat16 [64, 2048], P('tp', 'kv'), may hold values from -20 to 20
- gain_before: float32 [2048], P('kv'), may hold values from 0.1 to 1.9
- gate_before: bfloat16 [2048, 5632], P('kv', 'tp'), may hold values from -0.125 to 0.125
- lift_before: bfloat16 [2048, 5632], P('kv', 'tp'), may hold values from -0.125 to 0.125
- drop_before: bfloat16 [5632, 2048], P('tp', 'kv'), may hold values from -0.078125 to 0.078125
- mixer_gain: float32 [2048], P('kv'), may hold values from 0.1 to 1.9
- value_proj: bfloat16 [2048, 2048], P('kv', 'tp'), may hold values from -0.125 to 0.125
- gate_proj: bfloat16 [2048, 2048], P('kv', 'tp'), may hold values from -0.125 to 0.125
- key_proj: bfloat16 [2048, 1024], P('kv', 'tp'), may hold values from -0.125 to 0.125
- query_proj: bfloat16 [2048, 1024], P('kv', 'tp'), may hold values from -0.125 to 0.125
- step_proj: bfloat16 [2048, 32], P('kv'), may hold values from -0.125 to 0.125
- value_taps: float32 [4, 2048], P(None, 'tp'), may hold values from -3 to 3
- key_taps: float32 [4, 1024], P(None, 'tp'), may hold values from -3 to 3
- query_taps: float32 [4, 1024], P(None, 'tp'), may hold values from -3 to 3
- value_past: bfloat16 [64, 3, 2048], P('kv', None, 'tp'), may hold values from -6 to 6
- key_past: bfloat16 [64, 3, 1024], P('kv', None, 'tp'), may hold values from -6 to 6
- query_past: bfloat16 [64, 3, 1024], P('kv', None, 'tp'), may hold values from -6 to 6
- decay_rate: float32 [32], P('tp'), may hold values from 0.05 to 1
- block_state: float32 [64, 32, 64, 128], P('kv', 'tp'), may hold values from -24 to 24
- block_keys: bfloat16 [64, 128, 1024], P('kv', None, 'tp'), may hold values from -6 to 6
- block_values: bfloat16 [64, 128, 2048], P('kv', None, 'tp'), may hold values from -6 to 6
- block_steps: float32 [64, 128, 32], P('kv', None, 'tp'), may hold values from 0.2 to 2
- block_decay: float32 [64, 128, 32], P('kv', None, 'tp'), may hold values from -1.25 to 0
- lengths: int32 [64], P('kv'), may hold values from 1 to 128, 2048 in all
- head_gain: float32 [2048], P('tp'), may hold values from 0.1 to 1.9
- out_proj: bfloat16 [2048, 2048], P('tp', 'kv'), may hold values from -0.125 to 0.125
- gain_after: float32 [2048], P('kv'), may hold values from 0.1 to 1.9
- gate_after: bfloat16 [2048, 5632], P('kv', 'tp'), may hold values from -0.125 to 0.125
- lift_after: bfloat16 [2048, 5632], P('kv', 'tp'), may hold values from -0.125 to 0.125
- drop_after: bfloat16 [5632, 2048], P('tp', 'kv'), may hold values from -0.078125 to 0.078125
Outputs:
- hidden_out: bfloat16 [64, 2048], P('tp', 'kv')
The draws below stay inside these ranges and needn't reach their ends.
Inputs may be any that keep to these rules, and one draw needn't show every extreme that they name: `lengths`: some sequence has all 128 positions filled.
All inputs are finite; a program needn't handle non-finite values. No bound on the sum of `lengths` on one device may be relied on, other than what follows from the above.
Results may differ from the reference program's by a relative error of at most 0.014.
Values may be sent and summed in bfloat16 or wider, within the bound.
A program may use at most 64 MiB of HBM per device.

```python
import math
import jax
import jax.numpy as jnp
import numpy as np
from jax import lax

D = 2048
FF = 5632
HEAD_DIM = 64
STATE = 128
GROUPS = 8
BLOCK_POSITIONS = 128
CONV = 4
HEADS = 32
SEQUENCE_TOTAL = 64
N_TP = 2


def draw_hidden_in(key, part):
    first_key = jax.random.fold_in(jax.random.fold_in(key, 11), 0)
    column = jnp.arange(D, dtype=jnp.float32) / D
    draws = jnp.clip(jax.random.normal(first_key, (SEQUENCE_TOTAL, D), jnp.float32), -6.0, 6.0)
    values = draws * jnp.exp(column * jnp.log(3.0))[None, :]
    return values.astype(jnp.bfloat16)


def draw_block_decay(key, part):
    random_key_table = jax.random.split(jax.random.fold_in(key, 23), 7)
    fast_share = 0.5
    fast_heads = jax.random.uniform(random_key_table[0], (HEADS,), jnp.float32) < fast_share
    fast_rate = jax.random.uniform(random_key_table[1], (HEADS,), jnp.float32, 2.5, 4.5) / BLOCK_POSITIONS
    slow_rate = jax.random.uniform(random_key_table[2], (HEADS,), jnp.float32, 0.2, 1.0) / BLOCK_POSITIONS
    head_rate = jnp.where(fast_heads, fast_rate, slow_rate)
    seq_factor = jnp.exp(jax.random.uniform(random_key_table[3], (SEQUENCE_TOTAL, 1, 1), jnp.float32, jnp.log(0.6), jnp.log(1.4)))
    jitter = jax.random.uniform(random_key_table[4], (SEQUENCE_TOTAL, BLOCK_POSITIONS, HEADS), jnp.float32, 0.5, 1.5)
    position_within_block = jax.random.randint(random_key_table[5], (SEQUENCE_TOTAL, 2), 0, BLOCK_POSITIONS)
    token_position = jnp.arange(BLOCK_POSITIONS, dtype=jnp.int32)
    matched_mask = jnp.any(token_position[None, :, None] == position_within_block[:, None, :], axis=2)
    keep_share = jax.random.uniform(random_key_table[6], (SEQUENCE_TOTAL, BLOCK_POSITIONS, HEADS), jnp.float32, 0.55, 0.8)
    values = -head_rate[None, None, :] * seq_factor * jitter + jnp.where(matched_mask[:, :, None], jnp.log(keep_share), 0.0)
    return values.astype(jnp.float32)


def block_levels(stream_key, shape, cuts, least, high):
    level, own = 1.0, jax.random.fold_in(stream_key, 6)
    for dim, blocks in cuts:
        steps = jnp.exp(jax.random.uniform(jax.random.fold_in(own, dim), (blocks,), jnp.float32, least / len(cuts), high / len(cuts)))
        level = level * jnp.repeat(steps, shape[dim] // blocks).reshape([-1 if axis == dim else 1 for axis in range(len(shape))])
    return level


def profile(number_of, total, limit, slope):
    weights = [(1 << 20) // math.isqrt(grade ** slope) + 1 for grade in range(2, number_of + 1)]
    spare, given = total - limit - (number_of - 1), [1] * (number_of - 1)
    while spare > 0:
        free = [i for i in range(number_of - 1) if given[i] < limit]
        whole, budget = sum([weights[i] for i in free]), spare
        for i in free:
            more = min(limit - given[i], max(1, budget * weights[i] // whole), spare)
            given[i] = given[i] + more
            spare = spare - more
    return np.array([limit] + given)


def uneven(key, number_of, total, limit, skew):
    if number_of == 2:
        one = jax.random.randint(key, (), max(1, total - limit), min(limit, total - 1) + 1)
        return jnp.stack([one, total - one])
    sizes = jnp.asarray(profile(number_of, total, limit, skew), jnp.int32)
    pairs = (number_of - 1) // 2
    donor, sink = sizes[1:1 + 2 * pairs:2], sizes[2:2 + 2 * pairs:2]
    margin = jnp.minimum(donor - 1, limit - sink)
    shifted = jax.random.randint(jax.random.fold_in(key, 1), (pairs,), 0, 1 << 20) % (margin + 1)
    sizes = sizes.at[1:1 + 2 * pairs:2].set(donor - shifted).at[2:2 + 2 * pairs:2].set(sink + shifted)
    return sizes[jax.random.permutation(jax.random.fold_in(key, 2), number_of)]


def scatter_about(stream_key, shape, deviation, most, cuts=(), kind=jnp.bfloat16):
    array = jax.random.normal(stream_key, shape, jnp.float32) * deviation
    if len(cuts) > 0:
        array = block_levels(stream_key, shape, cuts, -0.22, 0.18) * array
    return jnp.clip(array, min=-most, max=most).astype(kind)


def setup_inputs(seed: int = 0) -> dict:
    keys = jax.random.split(jax.random.key(seed), 31)
    return {
        "hidden_in": draw_hidden_in(jax.random.fold_in(keys[30], 71), 0),
        "gain_before": jnp.clip(1.0 + 0.18 * jax.random.normal(keys[1], (D,), jnp.float32), 0.1, 1.9),
        "gate_before": scatter_about(keys[2], (D, FF), D ** -0.5, 0.125, ((0, 16), (1, 2))),
        "lift_before": scatter_about(keys[3], (D, FF), D ** -0.5, 0.125, ((0, 16), (1, 2))),
        "drop_before": scatter_about(keys[4], (FF, D), FF ** -0.5, 0.078125, ((0, 2), (1, 16))),
        "mixer_gain": jnp.clip(1.0 + 0.18 * jax.random.normal(keys[5], (D,), jnp.float32), 0.1, 1.9),
        "value_proj": scatter_about(keys[6], (D, D), D ** -0.5, 0.125, ((0, 16), (1, 2))),
        "gate_proj": scatter_about(keys[7], (D, D), D ** -0.5, 0.125, ((0, 16), (1, 2))),
        "key_proj": scatter_about(keys[8], (D, GROUPS * STATE), D ** -0.5, 0.125, ((0, 16), (1, 2))),
        "query_proj": scatter_about(keys[9], (D, GROUPS * STATE), D ** -0.5, 0.125, ((0, 16), (1, 2))),
        "step_proj": scatter_about(keys[10], (D, HEADS), D ** -0.5, 0.125, ((0, 16),)),
        "value_taps": scatter_about(keys[11], (CONV, D), 0.5, 3.0, ((1, 2),), jnp.float32),
        "key_taps": scatter_about(keys[12], (CONV, GROUPS * STATE), 0.5, 3.0, ((1, 2),), jnp.float32),
        "query_taps": scatter_about(keys[13], (CONV, GROUPS * STATE), 0.5, 3.0, ((1, 2),), jnp.float32),
        "value_past": scatter_about(keys[14], (SEQUENCE_TOTAL, CONV - 1, D), 1.0, 6.0, ((0, 16), (2, 2))),
        "key_past": scatter_about(keys[15], (SEQUENCE_TOTAL, CONV - 1, GROUPS * STATE), 1.0, 6.0, ((0, 16), (2, 2))),
        "query_past": scatter_about(keys[16], (SEQUENCE_TOTAL, CONV - 1, GROUPS * STATE), 1.0, 6.0, ((0, 16), (2, 2))),
        "decay_rate": jnp.clip(jnp.exp(math.log(1.0) - 2.9957323 * jax.random.uniform(keys[17], (HEADS,), jnp.float32) ** block_levels(keys[17], (HEADS,), ((0, 2),), -0.2, 0.2)), 0.05, 1.0),
        "block_state": scatter_about(keys[18], (SEQUENCE_TOTAL, HEADS, HEAD_DIM, STATE), 4.0, 24.0, ((0, 16), (1, 2)), jnp.float32),
        "block_keys": scatter_about(keys[19], (SEQUENCE_TOTAL, BLOCK_POSITIONS, GROUPS * STATE), 1.0, 6.0, ((0, 16), (2, 2))),
        "block_values": scatter_about(keys[20], (SEQUENCE_TOTAL, BLOCK_POSITIONS, D), 1.0, 6.0, ((0, 16), (2, 2))),
        "block_steps": jnp.clip(jnp.exp(math.log(2.0) - 2.3025851 * jax.random.uniform(keys[21], (SEQUENCE_TOTAL, BLOCK_POSITIONS, HEADS), jnp.float32) ** block_levels(keys[21], (SEQUENCE_TOTAL, BLOCK_POSITIONS, HEADS), ((0, 16), (2, 2)), -0.2, 0.2)), 0.2, 2.0),
        "block_decay": draw_block_decay(jax.random.fold_in(keys[30], 71), 0),
        "lengths": uneven(keys[23], SEQUENCE_TOTAL, SEQUENCE_TOTAL * BLOCK_POSITIONS // 4, BLOCK_POSITIONS, 2).astype(jnp.int32),
        "head_gain": jnp.clip(1.0 + 0.18 * jax.random.normal(keys[24], (D,), jnp.float32), 0.1, 1.9),
        "out_proj": scatter_about(keys[25], (D, D), D ** -0.5, 0.125, ((0, 2), (1, 16))),
        "gain_after": jnp.clip(1.0 + 0.18 * jax.random.normal(keys[26], (D,), jnp.float32), 0.1, 1.9),
        "gate_after": scatter_about(keys[27], (D, FF), D ** -0.5, 0.125, ((0, 16), (1, 2))),
        "lift_after": scatter_about(keys[28], (D, FF), D ** -0.5, 0.125, ((0, 16), (1, 2))),
        "drop_after": scatter_about(keys[29], (FF, D), FF ** -0.5, 0.078125, ((0, 2), (1, 16))),
    }


EPSILON = 1e-06

def inverse_rms(rows_in):
    values = rows_in.astype(jnp.float32)
    return lax.rsqrt(lax.optimization_barrier(jnp.mean(values * values, axis=1)) + EPSILON)[:, None]

def blocked_down(hidden, weight):
    inner = hidden.shape[1] // N_TP
    hidden_blocks = hidden.reshape(hidden.shape[0], N_TP, inner).astype(jnp.float32)
    weight_blocks = weight.reshape(N_TP, inner, weight.shape[1]).astype(jnp.float32)
    pieces = jnp.einsum('btf,tfd->tbd', hidden_blocks, weight_blocks, precision=lax.Precision.HIGHEST).astype(jnp.bfloat16)
    return lax.optimization_barrier(jnp.sum(pieces.astype(jnp.float32), axis=0))

def half_mlp(rows_in, gain_vec, gate_weight, lift_weight, drop_weight):
    row_scale = inverse_rms(rows_in)
    scaled = (rows_in.astype(jnp.float32) * gain_vec[None, :]).astype(jnp.bfloat16)
    gate_vals = row_scale * jnp.dot(scaled, gate_weight, preferred_element_type=jnp.float32)
    lift_vals = row_scale * jnp.dot(scaled, lift_weight, preferred_element_type=jnp.float32)
    hidden = (jax.nn.silu(gate_vals) * lift_vals).astype(jnp.bfloat16)
    return blocked_down(hidden, drop_weight)

def convolve(past_rows, taps, newest):
    earlier = lax.optimization_barrier(jnp.sum(past_rows.astype(jnp.float32) * taps[None, :-1, :], axis=1))
    return jax.nn.silu(earlier + taps[-1][None, :] * newest)

def mixer(rows_in, mixer_gain, value_proj, gate_proj, key_proj, query_proj, step_proj, value_taps, key_taps, query_taps, value_past, key_past, query_past, decay_rate, block_state, block_keys, block_values, block_steps, block_decay, lengths, head_gain, out_proj):
    row_scale = inverse_rms(rows_in)
    scaled = (rows_in.astype(jnp.float32) * mixer_gain[None, :]).astype(jnp.bfloat16)

    def project(weight):
        return row_scale * jnp.dot(scaled, weight, preferred_element_type=jnp.float32)
    new_value = convolve(value_past, value_taps, project(value_proj))
    gate_vals = project(gate_proj)
    new_key = convolve(key_past, key_taps, project(key_proj))
    new_query = convolve(query_past, query_taps, project(query_proj))
    step_size = jax.nn.softplus(project(step_proj))
    new_decay = -decay_rate[None, :] * step_size
    batch = rows_in.shape[0]
    block_len = block_keys.shape[1]
    per_group = HEADS // GROUPS
    live_mask = (jnp.arange(block_len, dtype=jnp.int32)[None, :] < (lengths - 1)[:, None])[:, :, None]
    masked = jnp.where(live_mask, block_decay, 0.0)
    running = jnp.cumsum(masked, axis=1)
    block_total = running[:, -1, :]
    tail_sum = block_total[:, None, :] - running
    query_round = new_query.astype(jnp.bfloat16).astype(jnp.float32)
    scores = jnp.einsum('blgn,bgn->blg', block_keys.reshape(batch, block_len, GROUPS, STATE).astype(jnp.float32), query_round.reshape(batch, GROUPS, STATE), precision=lax.Precision.HIGHEST)
    scores = jnp.repeat(scores, per_group, axis=2)
    weights = jnp.where(live_mask, jnp.exp(tail_sum + new_decay[:, None, :]) * block_steps * scores, 0.0).astype(jnp.bfloat16)
    from_block = jnp.einsum('blh,blhp->bhp', weights.astype(jnp.float32), block_values.reshape(batch, block_len, HEADS, HEAD_DIM).astype(jnp.float32), precision=lax.Precision.HIGHEST)
    query_heads = jnp.repeat(new_query.reshape(batch, GROUPS, STATE), per_group, axis=1)
    source_state = jnp.einsum('bhpn,bhn->bhp', block_state, query_heads, precision=lax.Precision.HIGHEST)
    source_state = source_state * jnp.exp(block_total + new_decay)[:, :, None]
    self_score = jnp.repeat(lax.optimization_barrier(jnp.sum((new_query * new_key).reshape(batch, GROUPS, STATE), axis=2)), per_group, axis=1)
    from_token = (step_size * self_score)[:, :, None] * new_value.reshape(batch, HEADS, HEAD_DIM)
    gated_out = (source_state + from_block + from_token) * jax.nn.silu(gate_vals.reshape(batch, HEADS, HEAD_DIM))
    normed = gated_out * lax.rsqrt(lax.optimization_barrier(jnp.mean(gated_out * gated_out, axis=2, keepdims=True)) + EPSILON)
    normed = normed * head_gain.reshape(HEADS, HEAD_DIM)[None]
    mixed_rows = normed.reshape(batch, HEADS * HEAD_DIM).astype(jnp.bfloat16)
    return blocked_down(mixed_rows, out_proj)

def reference(hidden_in, gain_before, gate_before, lift_before, drop_before, mixer_gain, value_proj, gate_proj, key_proj, query_proj, step_proj, value_taps, key_taps, query_taps, value_past, key_past, query_past, decay_rate, block_state, block_keys, block_values, block_steps, block_decay, lengths, head_gain, out_proj, gain_after, gate_after, lift_after, drop_after):
    section_one = (hidden_in.astype(jnp.float32) + 0.5 * half_mlp(hidden_in, gain_before, gate_before, lift_before, drop_before)).astype(jnp.bfloat16)
    branch_mix = mixer(section_one, mixer_gain, value_proj, gate_proj, key_proj, query_proj, step_proj, value_taps, key_taps, query_taps, value_past, key_past, query_past, decay_rate, block_state, block_keys, block_values, block_steps, block_decay, lengths, head_gain, out_proj)
    section_two = (section_one.astype(jnp.float32) + branch_mix).astype(jnp.bfloat16)
    return (section_two.astype(jnp.float32) + 0.5 * half_mlp(section_two, gain_after, gate_after, lift_after, drop_after)).astype(jnp.bfloat16)
```

```python
import functools
import math

import jax
import jax.numpy as jnp
from jax import lax
from jax.experimental import pallas as pl
from jax.experimental.pallas import tpu as pltpu
from jax.sharding import PartitionSpec as P

MESH_ID = pl.DeviceIdType.MESH
LANES = 128

D = 2048
GROUPS = 8
HEADS = 32


EPSILON = 1e-06


class Plan:
    def __init__(self, kv, rows, own_rows, width, hidden, seqs):
        inner = max(i for i in range(1, math.isqrt(kv) + 1) if kv % i == 0)
        self.kv, self.inner, self.outer = kv, inner, kv // inner
        self.rows, self.own_rows, self.width = rows, own_rows, width
        self.model = width * kv
        self.group = rows // inner
        self.seqs = seqs
        tiles = hidden // LANES
        wide = -(-tiles // self.outer)
        self.starts = [c * (tiles - wide) // max(self.outer - 1, 1) * LANES for c in range(self.outer)]
        self.tiles, self.wide_tiles = tiles, wide
        self.wide = wide * LANES
        ends = self.starts[1:] + [tiles * LANES]
        self.used = [e - s for s, e in zip(self.starts, ends)]

    def start(self, c):
        first = (c * (self.tiles - self.wide_tiles)) // max(self.outer - 1, 1)
        return pl.multiple_of(first * LANES, LANES)


def place(plan):
    k = lax.axis_index("kv")
    return lax.div(k, plan.inner), lax.rem(k, plan.inner), lax.axis_index("tp")


def greet(plan, z, p, t):
    barrier = pltpu.get_barrier_semaphore()
    for d in range(1, plan.inner):
        pl.semaphore_signal(barrier, inc=1, device_id=plane_peer(plan, z, p, t, d), device_id_type=MESH_ID)
    for d in range(1, plan.outer):
        pl.semaphore_signal(barrier, inc=1, device_id=line_peer(plan, z, p, t, d), device_id_type=MESH_ID)
    pl.semaphore_signal(barrier, inc=1, device_id=(z * plan.inner + p, 1 - t), device_id_type=MESH_ID)
    pl.semaphore_wait(barrier, plan.inner + plan.outer - 1)


def plane_peer(plan, z, p, t, d):
    return (z * plan.inner + lax.rem(p + d, plan.inner), t)


def line_peer(plan, z, p, t, d):
    return (lax.rem(z + d, plan.outer) * plan.inner + p, t)


def remote(src, dst, sems, index, device):
    return pltpu.make_async_remote_copy(
        src_ref=src,
        dst_ref=dst,
        send_sem=sems.at[(0,) + index],
        recv_sem=sems.at[(1,) + index],
        device_id=device,
        device_id_type=MESH_ID,
    )


def silu(a):
    return a / (1.0 + jnp.exp(-a))


def unit_scratch(plan):
    span = 2 * plan.wide + LANES
    i, o, g = plan.inner, plan.outer, plan.group
    return [
        pltpu.VMEM((i, o, g, span), jnp.bfloat16),
        pltpu.VMEM((i, o, g, span), jnp.bfloat16),
        pltpu.VMEM((o, g, span), jnp.bfloat16),
        pltpu.VMEM((o, g, span), jnp.bfloat16),
        pltpu.VMEM((o, i, g, plan.wide), jnp.bfloat16),
        pltpu.SemaphoreType.DMA((2, i, o)),
        pltpu.SemaphoreType.DMA((2, o)),
        pltpu.SemaphoreType.DMA((2, o)),
        pltpu.SemaphoreType.DMA((2, i, o)),
    ]


def unit_product(plan, x, gain, gate_ref, lift_ref, drop_ref, scratch):
    out_buf, in_buf, line_out, line_in, hid, plane_sem, line_sem, hz_sem, hp_sem = scratch
    z, p, t = place(plan)
    inner, outer, group, wide = plan.inner, plan.outer, plan.group, plan.wide
    values = x.astype(jnp.float32)
    squares = jnp.sum(values * values, axis=1, keepdims=True)
    squares = jnp.broadcast_to(squares, (plan.rows, LANES)).astype(jnp.bfloat16)
    scaled = (values * gain).astype(jnp.bfloat16)
    sends = []
    plane = []
    for n in range(outer):
        c = lax.rem(z + 1 + n, outer)
        columns = pl.ds(plan.start(c), wide)
        gate = jnp.dot(scaled, gate_ref[:, columns], preferred_element_type=jnp.float32).astype(jnp.bfloat16)
        lift = jnp.dot(scaled, lift_ref[:, columns], preferred_element_type=jnp.float32).astype(jnp.bfloat16)
        for q in range(inner):
            rows = slice(q * group, (q + 1) * group)
            out_buf[q, n, :, 0:wide] = gate[rows]
            out_buf[q, n, :, wide : 2 * wide] = lift[rows]
            out_buf[q, n, :, 2 * wide :] = squares[rows]
        copies = []
        for d in range(1, inner):
            copy = remote(
                out_buf.at[lax.rem(p + d, inner), n],
                in_buf.at[d, n],
                plane_sem,
                (d, n),
                plane_peer(plan, z, p, t, d),
            )
            copy.start()
            copies.append(copy)
        plane.append(copies)
        sends.extend(copies)
    line = []
    for n in range(outer):
        total = out_buf[p, n].astype(jnp.float32)
        for d in range(1, inner):
            plane[n][d - 1].wait_recv()
            total = total + in_buf[d, n].astype(jnp.float32)
        if n < outer - 1:
            line_out[n] = total.astype(jnp.bfloat16)
            copy = remote(line_out.at[n], line_in.at[n], line_sem, (n,), line_peer(plan, z, p, t, n + 1))
            copy.start()
            line.append(copy)
    sends.extend(line)
    for n in range(outer - 1):
        line[n].wait_recv()
        total = total + line_in[n].astype(jnp.float32)
    scale = lax.rsqrt(total[:, 2 * wide :] / plan.model + EPSILON)[:, 0:1]
    hidden = silu(total[:, 0:wide] * scale) * (total[:, wide : 2 * wide] * scale)
    hid[z, p] = hidden.astype(jnp.bfloat16)
    line = []
    for d in range(1, outer):
        copy = remote(hid.at[z, p], hid.at[z, p], hz_sem, (d,), line_peer(plan, z, p, t, d))
        copy.start()
        line.append(copy)
    sends.extend(line)

    def from_line(d):
        source = lax.rem(z + outer - d, outer)
        return remote(hid.at[source, p], hid.at[source, p], hz_sem, (d,), line_peer(plan, z, p, t, d))

    for n in range(outer):
        source = lax.rem(z + outer - n, outer)
        if n > 0:
            from_line(n).wait_recv()
        for d in range(1, inner):
            copy = remote(hid.at[source, p], hid.at[source, p], hp_sem, (d, n), plane_peer(plan, z, p, t, d))
            copy.start()
            sends.append(copy)
    for n in range(outer):
        source = lax.rem(z + outer - n, outer)
        for d in range(1, inner):
            sender = lax.rem(p + inner - d, inner)
            remote(
                hid.at[source, sender], hid.at[source, sender], hp_sem, (d, n), plane_peer(plan, z, p, t, d)
            ).wait_recv()
    total = jnp.zeros((plan.rows, plan.width), jnp.float32)
    for c in range(outer):
        first, used = plan.starts[c], plan.used[c]
        lhs = hid[c, :, :, 0:used].reshape(plan.rows, used)
        total = total + jnp.dot(lhs, drop_ref[first : first + used, :], preferred_element_type=jnp.float32)
    return total.astype(jnp.bfloat16), sends


def swap_whole(plan, mine, pair, sem):
    z, p, t = place(plan)
    pair[0] = mine
    copy = remote(pair.at[0], pair.at[1], sem, (0,), (z * plan.inner + p, 1 - t))
    copy.start()
    copy.wait()
    return mine.astype(jnp.float32) + pair[1].astype(jnp.float32)


def first_kernel(
    plan,
    x_ref,
    gain_ref,
    gate_ref,
    lift_ref,
    drop_ref,
    mix_gain_ref,
    value_ref,
    mgate_ref,
    key_ref,
    query_ref,
    step_ref,
    section_ref,
    raw_ref,
    gathered,
    gather_sem,
    pair,
    pair_sem,
    mix_out,
    mix_in,
    mline_out,
    mline_in,
    mplane_sem,
    mline_sem,
    *scratch,
):
    z, p, t = place(plan)
    inner, outer, group, seqs = plan.inner, plan.outer, plan.group, plan.seqs
    greet(plan, z, p, t)
    copy = remote(x_ref, gathered.at[t], gather_sem, (0,), (z * inner + p, 1 - t))
    copy.start()
    gathered[t] = x_ref[...]
    remote(x_ref, gathered.at[1 - t], gather_sem, (0,), (z * inner + p, 1 - t)).wait_recv()
    x = gathered[...].reshape(plan.rows, plan.width)
    product, sends = unit_product(plan, x, gain_ref[...], gate_ref, lift_ref, drop_ref, scratch)
    sends.append(copy)
    unit = swap_whole(plan, product, pair, pair_sem)
    section = (x.astype(jnp.float32) + 0.5 * unit).astype(jnp.bfloat16)
    section_ref[...] = section
    at = lax.broadcasted_iota(jnp.int32, (plan.rows, plan.rows), 0)
    of = lax.broadcasted_iota(jnp.int32, (plan.rows, plan.rows), 1)
    own_inner = lax.div(at, outer * seqs)
    rest = at - own_inner * (outer * seqs)
    own_outer = lax.div(rest, seqs)
    wanted = (own_outer * inner + own_inner) * seqs + (rest - own_outer * seqs)
    moving = jnp.where(of == wanted, 1.0, 0.0).astype(jnp.bfloat16)
    values = jnp.dot(moving, section, preferred_element_type=jnp.float32)
    squares = jnp.sum(values * values, axis=1, keepdims=True)
    scaled = (values * mix_gain_ref[...]).astype(jnp.bfloat16)
    steps = step_ref.shape[1]
    row = lax.broadcasted_iota(jnp.int32, (steps, LANES), 0)
    lane = lax.broadcasted_iota(jnp.int32, (steps, LANES), 1)
    spread = jnp.where(row == lane, 1.0, 0.0).astype(jnp.bfloat16)
    step_wide = jnp.dot(step_ref[...], spread, preferred_element_type=jnp.float32).astype(jnp.bfloat16)
    lanes = lax.broadcasted_iota(jnp.int32, (plan.rows, LANES), 1)
    last = jnp.dot(scaled, step_wide, preferred_element_type=jnp.float32)
    last = jnp.where(lanes == LANES - 1, squares, last).astype(jnp.bfloat16)
    chunks, first = [], 0
    plane = []
    for n, refs in enumerate(((key_ref, query_ref), (value_ref,), (mgate_ref,))):
        low = first
        pieces = [jnp.dot(scaled, ref[...], preferred_element_type=jnp.float32).astype(jnp.bfloat16) for ref in refs]
        if n == 0:
            pieces.append(last)
        for piece in pieces:
            size = piece.shape[1]
            for q in range(inner):
                mix_out[q, :, first : first + size] = piece[q * group : (q + 1) * group]
            first = first + size
        columns = slice(low, first)
        chunks.append(columns)
        copies = []
        for d in range(1, inner):
            copy = remote(
                mix_out.at[lax.rem(p + d, inner), :, columns],
                mix_in.at[d, :, columns],
                mplane_sem,
                (d, n),
                plane_peer(plan, z, p, t, d),
            )
            copy.start()
            copies.append(copy)
        plane.append(copies)
        sends.extend(copies)
    line = []
    for n, columns in enumerate(chunks):
        total = mix_out[p, :, columns].astype(jnp.float32)
        for d in range(1, inner):
            plane[n][d - 1].wait_recv()
            total = total + mix_in[d, :, columns].astype(jnp.float32)
        for o in range(outer):
            mline_out[o, :, columns] = total[o * seqs : (o + 1) * seqs]
        copies = []
        for d in range(1, outer):
            copy = remote(
                mline_out.at[lax.rem(z + d, outer), :, columns],
                mline_in.at[d, :, columns],
                mline_sem,
                (d, n),
                line_peer(plan, z, p, t, d),
            )
            copy.start()
            copies.append(copy)
        line.append(copies)
        sends.extend(copies)
    scale = None
    for n, columns in enumerate(chunks):
        total = mline_out[z, :, columns]
        for d in range(1, outer):
            line[n][d - 1].wait_recv()
            total = total + mline_in[d, :, columns]
        if n == 0:
            scale = lax.rsqrt(total[:, -1:] / plan.model + EPSILON)
        raw_ref[:, columns] = total * scale
    for copy in sends:
        copy.wait_send()


def last_kernel(
    plan,
    section_ref,
    mixed_ref,
    out_proj_ref,
    gain_ref,
    gate_ref,
    lift_ref,
    drop_ref,
    out_ref,
    mixed,
    stacked,
    pair,
    final_in,
    final_out,
    section_buf,
    mz_sem,
    mp_sem,
    pair_sem,
    final_sem,
    *scratch,
):
    z, p, t = place(plan)
    inner, outer, seqs = plan.inner, plan.outer, plan.seqs
    greet(plan, z, p, t)
    sends = []
    for d in range(1, outer):
        copy = remote(mixed_ref, mixed.at[z, p], mz_sem, (d,), line_peer(plan, z, p, t, d))
        copy.start()
        sends.append(copy)
    for n in range(outer):
        source = lax.rem(z + outer - n, outer)
        block = mixed_ref if n == 0 else mixed.at[source, p]
        if n > 0:
            remote(block, mixed.at[source, p], mz_sem, (n,), line_peer(plan, z, p, t, n)).wait_recv()
        for d in range(1, inner):
            copy = remote(block, mixed.at[source, p], mp_sem, (d, n), plane_peer(plan, z, p, t, d))
            copy.start()
            sends.append(copy)
    mixed[z, p] = mixed_ref[...]
    for n in range(outer):
        source = lax.rem(z + outer - n, outer)
        for d in range(1, inner):
            sender = lax.rem(p + inner - d, inner)
            remote(
                mixed_ref, mixed.at[source, sender], mp_sem, (d, n), plane_peer(plan, z, p, t, d)
            ).wait_recv()
    for o in range(outer):
        for i in range(inner):
            first = (o * inner + i) * seqs
            stacked[first : first + seqs, :] = mixed[o, i]
    product = jnp.dot(
        stacked[...].astype(jnp.bfloat16), out_proj_ref[...], preferred_element_type=jnp.float32
    ).astype(jnp.bfloat16)
    branch = swap_whole(plan, product, pair, pair_sem)
    x = (section_ref[...].astype(jnp.float32) + branch).astype(jnp.bfloat16)
    section_buf[...] = x.reshape(section_buf.shape)
    product, more = unit_product(plan, x, gain_ref[...], gate_ref, lift_ref, drop_ref, scratch)
    final_out[...] = product.reshape(final_out.shape)
    copy = remote(final_out.at[1 - t], final_in, final_sem, (0,), (z * inner + p, 1 - t))
    copy.start()
    copy.wait()
    unit = final_out[t].astype(jnp.float32) + final_in[...].astype(jnp.float32)
    out_ref[...] = (section_buf[t].astype(jnp.float32) + 0.5 * unit).astype(jnp.bfloat16)
    for copy in sends + more:
        copy.wait_send()


def run_first(plan, x, gain, gate, lift, drop, mix_gain, value, mgate, key, query, step):
    span = value.shape[1] + mgate.shape[1] + key.shape[1] + query.shape[1] + LANES
    i, o, g, s = plan.inner, plan.outer, plan.group, plan.seqs
    vmem = pl.BlockSpec(memory_space=pltpu.VMEM)
    return pl.pallas_call(
        functools.partial(first_kernel, plan),
        out_shape=(
            jax.ShapeDtypeStruct((plan.rows, plan.width), jnp.bfloat16),
            jax.ShapeDtypeStruct((s, span), jnp.float32),
        ),
        in_specs=[vmem] * 11,
        out_specs=(vmem, vmem),
        scratch_shapes=[
            pltpu.VMEM((2, plan.own_rows, plan.width), jnp.bfloat16),
            pltpu.SemaphoreType.DMA((2, 1)),
            pltpu.VMEM((2, plan.rows, plan.width), jnp.bfloat16),
            pltpu.SemaphoreType.DMA((2, 1)),
            pltpu.VMEM((i, g, span), jnp.bfloat16),
            pltpu.VMEM((i, g, span), jnp.bfloat16),
            pltpu.VMEM((o, s, span), jnp.float32),
            pltpu.VMEM((o, s, span), jnp.float32),
            pltpu.SemaphoreType.DMA((2, i, 3)),
            pltpu.SemaphoreType.DMA((2, o, 3)),
        ]
        + unit_scratch(plan),
        compiler_params=pltpu.CompilerParams(collective_id=0, has_side_effects=True),
        name="unit_and_projections",
    )(x, gain[None], gate, lift, drop, mix_gain[None], value, mgate, key, query, step)


def run_last(plan, section, mixed_rows, out_proj, gain, gate, lift, drop):
    i, o, s = plan.inner, plan.outer, plan.seqs
    vmem = pl.BlockSpec(memory_space=pltpu.VMEM)
    inner_width = out_proj.shape[0]
    return pl.pallas_call(
        functools.partial(last_kernel, plan),
        out_shape=jax.ShapeDtypeStruct((plan.own_rows, plan.width), jnp.bfloat16),
        in_specs=[vmem] * 7,
        out_specs=vmem,
        scratch_shapes=[
            pltpu.VMEM((o, i, s, inner_width), jnp.float32),
            pltpu.VMEM((plan.rows, inner_width), jnp.float32),
            pltpu.VMEM((2, plan.rows, plan.width), jnp.bfloat16),
            pltpu.VMEM((plan.own_rows, plan.width), jnp.bfloat16),
            pltpu.VMEM((2, plan.own_rows, plan.width), jnp.bfloat16),
            pltpu.VMEM((2, plan.own_rows, plan.width), jnp.bfloat16),
            pltpu.SemaphoreType.DMA((2, o)),
            pltpu.SemaphoreType.DMA((2, i, o)),
            pltpu.SemaphoreType.DMA((2, 1)),
            pltpu.SemaphoreType.DMA((2, 1)),
        ]
        + unit_scratch(plan),
        compiler_params=pltpu.CompilerParams(collective_id=1, has_side_effects=True),
        name="mix_out_and_unit",
    )(section, mixed_rows, out_proj, gain[None], gate, lift, drop)


def gather_rows(rows_in, gain_vec):
    whole_rows = lax.all_gather(rows_in, "tp", axis=0, tiled=True)
    values = whole_rows.astype(jnp.float32)
    squares = jnp.sum(values * values, axis=1)
    scaled = (values * gain_vec[None, :]).astype(jnp.bfloat16)
    return (scaled, squares)


def inverse_scale(totals):
    return lax.rsqrt(totals / D + EPSILON)[:, None]


def own_rows(totals, row_count):
    return lax.dynamic_slice_in_dim(totals, lax.axis_index("kv") * row_count, row_count, 0)


def finish(partial_value):
    return lax.psum_scatter(
        partial_value.astype(jnp.float32).astype(jnp.bfloat16),
        "tp",
        scatter_dimension=0,
        tiled=True,
    ).astype(jnp.float32)


def half_mlp(rows_in, gain_vec, gate_weight, lift_weight, drop_weight):
    scaled, squares = gather_rows(rows_in, gain_vec)
    totals = lax.psum(squares, "kv")
    gate_part = jnp.dot(scaled, gate_weight, preferred_element_type=jnp.float32)
    lift_part = jnp.dot(scaled, lift_weight, preferred_element_type=jnp.float32)
    gate_sum, lift_sum = lax.psum((gate_part, lift_part), "kv")
    row_scale = inverse_scale(totals)
    hidden = (jax.nn.silu(gate_sum * row_scale) * (lift_sum * row_scale)).astype(jnp.bfloat16)
    partial_value = jnp.dot(hidden, drop_weight, preferred_element_type=jnp.float32).astype(
        jnp.bfloat16
    )
    return finish(partial_value)


def convolve(past_rows, taps, newest):
    earlier = jnp.sum(past_rows.astype(jnp.float32) * taps[None, :-1, :], axis=1)
    return jax.nn.silu(earlier + taps[-1][None, :] * newest)


def mixer(
    rows_in,
    mixer_gain,
    value_proj,
    gate_proj,
    key_proj,
    query_proj,
    step_proj,
    value_taps,
    key_taps,
    query_taps,
    value_past,
    key_past,
    query_past,
    decay_rate,
    block_state,
    block_keys,
    block_values,
    block_steps,
    block_decay,
    lengths,
    head_gain,
    out_proj,
):
    scaled, squares = gather_rows(rows_in, mixer_gain)
    seq_count = lengths.shape[0]
    value_part = jnp.dot(scaled, value_proj, preferred_element_type=jnp.float32)
    gate_part = jnp.dot(scaled, gate_proj, preferred_element_type=jnp.float32)
    key_part = jnp.dot(scaled, key_proj, preferred_element_type=jnp.float32)
    query_part = jnp.dot(scaled, query_proj, preferred_element_type=jnp.float32)
    step_part = jnp.dot(scaled, step_proj, preferred_element_type=jnp.float32)
    totals = own_rows(lax.psum(squares, "kv"), seq_count)
    value_raw, gate_raw, key_raw, query_raw, step_all = (
        lax.psum_scatter(value_part, "kv", scatter_dimension=0, tiled=True),
        lax.psum_scatter(gate_part, "kv", scatter_dimension=0, tiled=True),
        lax.psum_scatter(key_part, "kv", scatter_dimension=0, tiled=True),
        lax.psum_scatter(query_part, "kv", scatter_dimension=0, tiled=True),
        lax.psum_scatter(step_part, "kv", scatter_dimension=0, tiled=True),
    )
    row_scale = inverse_scale(totals)
    heads_here = decay_rate.shape[0]
    step_raw = (
        lax.dynamic_slice_in_dim(step_all, lax.axis_index("tp") * heads_here, heads_here, 1)
        * row_scale
    )
    new_value = convolve(value_past, value_taps, value_raw * row_scale)
    gate_vals = gate_raw * row_scale
    new_key = convolve(key_past, key_taps, key_raw * row_scale)
    new_query = convolve(query_past, query_taps, query_raw * row_scale)
    step_size = jax.nn.softplus(step_raw)
    new_decay = -decay_rate[None, :] * step_size
    block_len = block_keys.shape[1]
    head_dim = block_state.shape[2]
    state_size = block_state.shape[3]
    per_group = HEADS // GROUPS
    group_count = heads_here // per_group
    live_mask = (jnp.arange(block_len, dtype=jnp.int32)[None, :] < (lengths - 1)[:, None])[
        :, :, None
    ]
    masked = jnp.where(live_mask, block_decay, 0.0)
    running = jnp.cumsum(masked, axis=1)
    block_total = running[:, -1, :]
    tail_sum = block_total[:, None, :] - running
    query_round = new_query.astype(jnp.bfloat16).reshape(seq_count, group_count, state_size)
    scores = jnp.einsum(
        "slgn,sgn->slg",
        block_keys.reshape(seq_count, block_len, group_count, state_size),
        query_round,
        preferred_element_type=jnp.float32,
    )
    scores = jnp.repeat(scores, per_group, axis=2)
    weights = jnp.where(
        live_mask, jnp.exp(tail_sum + new_decay[:, None, :]) * block_steps * scores, 0.0
    ).astype(jnp.bfloat16)
    from_block = jnp.einsum(
        "slh,slhp->shp",
        weights,
        block_values.reshape(seq_count, block_len, heads_here, head_dim),
        preferred_element_type=jnp.float32,
    )
    query_heads = jnp.repeat(
        new_query.reshape(seq_count, group_count, state_size), per_group, axis=1
    )
    source_state = jnp.einsum(
        "shpn,shn->shp", block_state, query_heads, precision=lax.Precision.HIGHEST
    )
    source_state = source_state * jnp.exp(block_total + new_decay)[:, :, None]
    self_score = jnp.repeat(
        jnp.sum((new_query * new_key).reshape(seq_count, group_count, state_size), axis=2),
        per_group,
        axis=1,
    )
    from_token = (step_size * self_score)[:, :, None] * new_value.reshape(
        seq_count, heads_here, head_dim
    )
    gated_out = (source_state + from_block + from_token) * jax.nn.silu(
        gate_vals.reshape(seq_count, heads_here, head_dim)
    )
    normed = gated_out * lax.rsqrt(jnp.mean(gated_out * gated_out, axis=2, keepdims=True) + EPSILON)
    normed = normed * head_gain.reshape(heads_here, head_dim)[None]
    mixed_rows = normed.reshape(seq_count, heads_here * head_dim).astype(jnp.bfloat16)
    partial_value = jnp.dot(
        lax.all_gather(mixed_rows, "kv", axis=0, tiled=True),
        out_proj,
        preferred_element_type=jnp.float32,
    ).astype(jnp.bfloat16)
    return finish(partial_value)


def on_device(
    hidden_in,
    gain_before,
    gate_before,
    lift_before,
    drop_before,
    mixer_gain,
    value_proj,
    gate_proj,
    key_proj,
    query_proj,
    step_proj,
    value_taps,
    key_taps,
    query_taps,
    value_past,
    key_past,
    query_past,
    decay_rate,
    block_state,
    block_keys,
    block_values,
    block_steps,
    block_decay,
    lengths,
    head_gain,
    out_proj,
    gain_after,
    gate_after,
    lift_after,
    drop_after,
):
    section_one = (
        hidden_in.astype(jnp.float32)
        + 0.5 * half_mlp(hidden_in, gain_before, gate_before, lift_before, drop_before)
    ).astype(jnp.bfloat16)
    branch_mix = mixer(
        section_one,
        mixer_gain,
        value_proj,
        gate_proj,
        key_proj,
        query_proj,
        step_proj,
        value_taps,
        key_taps,
        query_taps,
        value_past,
        key_past,
        query_past,
        decay_rate,
        block_state,
        block_keys,
        block_values,
        block_steps,
        block_decay,
        lengths,
        head_gain,
        out_proj,
    )
    section_two = (section_one.astype(jnp.float32) + branch_mix).astype(jnp.bfloat16)
    return (
        section_two.astype(jnp.float32)
        + 0.5 * half_mlp(section_two, gain_after, gate_after, lift_after, drop_after)
    ).astype(jnp.bfloat16)


def mix_block(
    value_raw,
    gate_raw,
    key_raw,
    query_raw,
    step_raw,
    value_taps,
    key_taps,
    query_taps,
    value_past,
    key_past,
    query_past,
    decay_rate,
    block_state,
    block_keys,
    block_values,
    block_steps,
    block_decay,
    lengths,
    head_gain,
):
    seq_count = lengths.shape[0]
    heads_here = decay_rate.shape[0]
    new_value = convolve(value_past, value_taps, value_raw)
    gate_vals = gate_raw
    new_key = convolve(key_past, key_taps, key_raw)
    new_query = convolve(query_past, query_taps, query_raw)
    step_size = jax.nn.softplus(step_raw)
    new_decay = -decay_rate[None, :] * step_size
    block_len = block_keys.shape[1]
    head_dim = block_state.shape[2]
    state_size = block_state.shape[3]
    per_group = HEADS // GROUPS
    group_count = heads_here // per_group
    live_mask = (jnp.arange(block_len, dtype=jnp.int32)[None, :] < (lengths - 1)[:, None])[
        :, :, None
    ]
    masked = jnp.where(live_mask, block_decay, 0.0)
    running = jnp.cumsum(masked, axis=1)
    block_total = running[:, -1, :]
    tail_sum = block_total[:, None, :] - running
    query_round = new_query.astype(jnp.bfloat16).reshape(seq_count, group_count, state_size)
    scores = jnp.einsum(
        "slgn,sgn->slg",
        block_keys.reshape(seq_count, block_len, group_count, state_size),
        query_round,
        preferred_element_type=jnp.float32,
    )
    scores = jnp.repeat(scores, per_group, axis=2)
    weights = jnp.where(
        live_mask, jnp.exp(tail_sum + new_decay[:, None, :]) * block_steps * scores, 0.0
    ).astype(jnp.bfloat16)
    from_block = jnp.einsum(
        "slh,slhp->shp",
        weights,
        block_values.reshape(seq_count, block_len, heads_here, head_dim),
        preferred_element_type=jnp.float32,
    )
    query_heads = jnp.repeat(
        new_query.reshape(seq_count, group_count, state_size), per_group, axis=1
    )
    source_state = jnp.einsum(
        "shpn,shn->shp", block_state, query_heads, precision=lax.Precision.HIGHEST
    )
    source_state = source_state * jnp.exp(block_total + new_decay)[:, :, None]
    self_score = jnp.repeat(
        jnp.sum((new_query * new_key).reshape(seq_count, group_count, state_size), axis=2),
        per_group,
        axis=1,
    )
    from_token = (step_size * self_score)[:, :, None] * new_value.reshape(
        seq_count, heads_here, head_dim
    )
    gated_out = (source_state + from_block + from_token) * jax.nn.silu(
        gate_vals.reshape(seq_count, heads_here, head_dim)
    )
    normed = gated_out * lax.rsqrt(jnp.mean(gated_out * gated_out, axis=2, keepdims=True) + EPSILON)
    normed = normed * head_gain.reshape(heads_here, head_dim)[None]
    return normed.reshape(seq_count, heads_here * head_dim).astype(jnp.bfloat16)


def on_device_fast(
    hidden_in,
    gain_before,
    gate_before,
    lift_before,
    drop_before,
    mixer_gain,
    value_proj,
    gate_proj,
    key_proj,
    query_proj,
    step_proj,
    value_taps,
    key_taps,
    query_taps,
    value_past,
    key_past,
    query_past,
    decay_rate,
    block_state,
    block_keys,
    block_values,
    block_steps,
    block_decay,
    lengths,
    head_gain,
    out_proj,
    gain_after,
    gate_after,
    lift_after,
    drop_after,
):
    kv, tp = lax.axis_size("kv"), lax.axis_size("tp")
    own_rows, width = hidden_in.shape
    rows, hidden, seqs = own_rows * tp, gate_before.shape[1], lengths.shape[0]
    plan = Plan(kv, rows, own_rows, width, hidden, seqs)
    section, raw = run_first(
        plan,
        hidden_in,
        gain_before,
        gate_before,
        lift_before,
        drop_before,
        mixer_gain,
        value_proj,
        gate_proj,
        key_proj,
        query_proj,
        step_proj,
    )
    sizes = (key_proj.shape[1], query_proj.shape[1], LANES, value_proj.shape[1], gate_proj.shape[1])
    ends = [sum(sizes[: n + 1]) for n in range(len(sizes))]
    key_raw, query_raw, step_all, value_raw, gate_raw = (
        raw[:, end - size : end] for size, end in zip(sizes, ends)
    )
    heads_here = decay_rate.shape[0]
    step_raw = lax.dynamic_slice_in_dim(step_all, lax.axis_index("tp") * heads_here, heads_here, 1)
    mixed_rows = mix_block(
        value_raw,
        gate_raw,
        key_raw,
        query_raw,
        step_raw,
        value_taps,
        key_taps,
        query_taps,
        value_past,
        key_past,
        query_past,
        decay_rate,
        block_state,
        block_keys,
        block_values,
        block_steps,
        block_decay,
        lengths,
        head_gain,
    )
    return run_last(
        plan,
        section,
        mixed_rows.astype(jnp.float32),
        out_proj,
        gain_after,
        gate_after,
        lift_after,
        drop_after,
    )


def fits(
    hidden_in,
    gain_before,
    gate_before,
    lift_before,
    drop_before,
    mixer_gain,
    value_proj,
    gate_proj,
    key_proj,
    query_proj,
    step_proj,
    value_taps,
    key_taps,
    query_taps,
    value_past,
    key_past,
    query_past,
    decay_rate,
    block_state,
    block_keys,
    block_values,
    block_steps,
    block_decay,
    lengths,
    head_gain,
    out_proj,
    gain_after,
    gate_after,
    lift_after,
    drop_after,
):
    kv, tp = lax.axis_size("kv"), lax.axis_size("tp")
    own_rows, width = hidden_in.shape
    inner = max(i for i in range(1, math.isqrt(kv) + 1) if kv % i == 0)
    aligned = (
        gate_before.shape[1],
        width,
        value_proj.shape[1],
        gate_proj.shape[1],
        key_proj.shape[1],
        query_proj.shape[1],
    )
    return (
        tp == 2
        and inner > 1
        and all(size % LANES == 0 for size in aligned)
        and own_rows % 16 == 0
        and own_rows * tp % (16 * inner) == 0
        and lengths.shape[0] in (4, 8)
        and lengths.shape[0] * kv == own_rows * tp
        and step_proj.shape[1] < LANES
        and gate_before.shape[1] // LANES >= 2 * (kv // inner)
    )


def choose(*args):
    return on_device_fast(*args) if fits(*args) else on_device(*args)


def solution(mesh):
    return jax.shard_map(
        choose,
        mesh=mesh,
        in_specs=(
            P("tp", "kv"),
            P("kv"),
            P("kv", "tp"),
            P("kv", "tp"),
            P("tp", "kv"),
            P("kv"),
            P("kv", "tp"),
            P("kv", "tp"),
            P("kv", "tp"),
            P("kv", "tp"),
            P("kv", None),
            P(None, "tp"),
            P(None, "tp"),
            P(None, "tp"),
            P("kv", None, "tp"),
            P("kv", None, "tp"),
            P("kv", None, "tp"),
            P("tp"),
            P("kv", "tp", None, None),
            P("kv", None, "tp"),
            P("kv", None, "tp"),
            P("kv", None, "tp"),
            P("kv", None, "tp"),
            P("kv"),
            P("tp"),
            P("tp", "kv"),
            P("kv"),
            P("kv", "tp"),
            P("kv", "tp"),
            P("tp", "kv"),
        ),
        out_specs=P("tp", "kv"),
        check_vma=False,
    )
```

```python
import functools
import math

import jax
import jax.numpy as jnp
from jax import lax
from jax.experimental import pallas as pl
from jax.experimental.pallas import tpu as pltpu
from jax.sharding import PartitionSpec as P

MESH_ID = pl.DeviceIdType.MESH
LANES = 128
SHORT = jnp.bfloat16

D = 2048
GROUPS = 8
HEADS = 32


EPSILON = 1e-06


class Plan:
    def __init__(self, kv, rows, own_rows, width, hidden, seqs):
        inner = max(i for i in range(1, math.isqrt(kv) + 1) if kv % i == 0)
        self.kv, self.inner, self.outer = kv, inner, kv // inner
        self.rows, self.own_rows, self.width = rows, own_rows, width
        self.model = width * kv
        self.group = rows // inner
        self.seqs = seqs
        tiles = hidden // LANES
        wide = -(-tiles // self.outer)
        self.starts = [c * (tiles - wide) // max(self.outer - 1, 1) * LANES for c in range(self.outer)]
        self.tiles, self.wide_tiles = tiles, wide
        self.wide = wide * LANES
        ends = self.starts[1:] + [tiles * LANES]
        self.used = [e - s for s, e in zip(self.starts, ends)]

    def start(self, c):
        first = (c * (self.tiles - self.wide_tiles)) // max(self.outer - 1, 1)
        return pl.multiple_of(first * LANES, LANES)


def place(plan):
    k = lax.axis_index("kv")
    return lax.div(k, plan.inner), lax.rem(k, plan.inner), lax.axis_index("tp")


def greet(plan, z, p, t):
    barrier = pltpu.get_barrier_semaphore()
    for d in range(1, plan.inner):
        pl.semaphore_signal(barrier, inc=1, device_id=plane_peer(plan, z, p, t, d), device_id_type=MESH_ID)
    for d in range(1, plan.outer):
        pl.semaphore_signal(barrier, inc=1, device_id=line_peer(plan, z, p, t, d), device_id_type=MESH_ID)
    pl.semaphore_signal(barrier, inc=1, device_id=(z * plan.inner + p, 1 - t), device_id_type=MESH_ID)
    pl.semaphore_wait(barrier, plan.inner + plan.outer - 1)


def plane_peer(plan, z, p, t, d):
    return (z * plan.inner + lax.rem(p + d, plan.inner), t)


def line_peer(plan, z, p, t, d):
    return (lax.rem(z + d, plan.outer) * plan.inner + p, t)


def remote(src, dst, sems, index, device):
    return pltpu.make_async_remote_copy(
        src_ref=src,
        dst_ref=dst,
        send_sem=sems.at[(0,) + index],
        recv_sem=sems.at[(1,) + index],
        device_id=device,
        device_id_type=MESH_ID,
    )


def silu(a):
    return a / (1.0 + jnp.exp(-a))


def unit_scratch(plan):
    span = 2 * plan.wide + LANES
    i, o, g = plan.inner, plan.outer, plan.group
    return [
        pltpu.VMEM((i, o, g, span), jnp.bfloat16),
        pltpu.VMEM((i, o, g, span), jnp.bfloat16),
        pltpu.VMEM((o, g, span), jnp.bfloat16),
        pltpu.VMEM((o, g, span), jnp.bfloat16),
        pltpu.VMEM((o, i, g, plan.wide), jnp.bfloat16),
        pltpu.SemaphoreType.DMA((2, i, o)),
        pltpu.SemaphoreType.DMA((2, o)),
        pltpu.SemaphoreType.DMA((2, o)),
        pltpu.SemaphoreType.DMA((2, i, o)),
    ]


def unit_product(plan, x, gain, gate_ref, lift_ref, drop_ref, scratch):
    out_buf, in_buf, line_out, line_in, hid, plane_sem, line_sem, hz_sem, hp_sem = scratch
    z, p, t = place(plan)
    inner, outer, group, wide = plan.inner, plan.outer, plan.group, plan.wide
    values = x.astype(jnp.float32)
    squares = jnp.sum(values * values, axis=1, keepdims=True)
    squares = jnp.broadcast_to(squares, (plan.rows, LANES)).astype(jnp.bfloat16)
    scaled = (values * gain).astype(jnp.bfloat16)
    sends = []
    plane = []
    for n in range(outer):
        c = lax.rem(z + 1 + n, outer)
        columns = pl.ds(plan.start(c), wide)
        gate = jnp.dot(scaled, gate_ref[:, columns], preferred_element_type=jnp.float32).astype(jnp.bfloat16)
        lift = jnp.dot(scaled, lift_ref[:, columns], preferred_element_type=jnp.float32).astype(jnp.bfloat16)
        for q in range(inner):
            rows = slice(q * group, (q + 1) * group)
            out_buf[q, n, :, 0:wide] = gate[rows]
            out_buf[q, n, :, wide : 2 * wide] = lift[rows]
            out_buf[q, n, :, 2 * wide :] = squares[rows]
        copies = []
        for d in range(1, inner):
            copy = remote(
                out_buf.at[lax.rem(p + d, inner), n],
                in_buf.at[d, n],
                plane_sem,
                (d, n),
                plane_peer(plan, z, p, t, d),
            )
            copy.start()
            copies.append(copy)
        plane.append(copies)
        sends.extend(copies)
    line = []
    for n in range(outer):
        total = out_buf[p, n].astype(jnp.float32)
        for d in range(1, inner):
            plane[n][d - 1].wait_recv()
            total = total + in_buf[d, n].astype(jnp.float32)
        if n < outer - 1:
            line_out[n] = total.astype(jnp.bfloat16)
            copy = remote(line_out.at[n], line_in.at[n], line_sem, (n,), line_peer(plan, z, p, t, n + 1))
            copy.start()
            line.append(copy)
    sends.extend(line)
    for n in range(outer - 1):
        line[n].wait_recv()
        total = total + line_in[n].astype(jnp.float32)
    scale = lax.rsqrt(total[:, 2 * wide :] / plan.model + EPSILON)[:, 0:1]
    hidden = silu(total[:, 0:wide] * scale) * (total[:, wide : 2 * wide] * scale)
    hid[z, p] = hidden.astype(jnp.bfloat16)
    line = []
    for d in range(1, outer):
        copy = remote(hid.at[z, p], hid.at[z, p], hz_sem, (d,), line_peer(plan, z, p, t, d))
        copy.start()
        line.append(copy)
    sends.extend(line)

    def from_line(d):
        source = lax.rem(z + outer - d, outer)
        return remote(hid.at[source, p], hid.at[source, p], hz_sem, (d,), line_peer(plan, z, p, t, d))

    for n in range(outer):
        source = lax.rem(z + outer - n, outer)
        if n > 0:
            from_line(n).wait_recv()
        for d in range(1, inner):
            copy = remote(hid.at[source, p], hid.at[source, p], hp_sem, (d, n), plane_peer(plan, z, p, t, d))
            copy.start()
            sends.append(copy)
    for n in range(outer):
        source = lax.rem(z + outer - n, outer)
        for d in range(1, inner):
            sender = lax.rem(p + inner - d, inner)
            remote(
                hid.at[source, sender], hid.at[source, sender], hp_sem, (d, n), plane_peer(plan, z, p, t, d)
            ).wait_recv()
    total = jnp.zeros((plan.rows, plan.width), jnp.float32)
    for c in range(outer):
        first, used = plan.starts[c], plan.used[c]
        lhs = hid[c, :, :, 0:used].reshape(plan.rows, used)
        total = total + jnp.dot(lhs, drop_ref[first : first + used, :], preferred_element_type=jnp.float32)
    return total.astype(jnp.bfloat16), sends


def swap_whole(plan, mine, pair, sem):
    z, p, t = place(plan)
    pair[0] = mine
    copy = remote(pair.at[0], pair.at[1], sem, (0,), (z * plan.inner + p, 1 - t))
    copy.start()
    copy.wait()
    return mine.astype(jnp.float32) + pair[1].astype(jnp.float32)


def block_mix(
    plan,
    raw,
    lengths_ref,
    vtap_ref,
    ktap_ref,
    qtap_ref,
    vpast_ref,
    kpast_ref,
    qpast_ref,
    rate_ref,
    head_gain_ref,
    state_high,
    state_low,
    keys_ref,
    values_ref,
    steps_ref,
    decay_ref,
    prepared,
):
    t = lax.axis_index("tp")
    heads, block_len = decay_ref.shape[1], decay_ref.shape[2]
    head_dim, states = state_high.shape[1] // heads, state_high.shape[2]
    groups = keys_ref.shape[2] // states
    per_group = heads // groups
    channels = heads * head_dim
    key_raw, query_raw, step_rows, value_raw, gate_rows = raw

    def convolve(past_ref, tap_ref, newest):
        last = tap_ref.shape[0] - 1
        total = tap_ref[last : last + 1, :] * newest
        for k in range(last):
            total = total + past_ref[k].astype(jnp.float32) * tap_ref[k : k + 1, :]
        return silu(total)

    new_value = convolve(vpast_ref, vtap_ref, value_raw)
    new_key = convolve(kpast_ref, ktap_ref, key_raw)
    new_query = convolve(qpast_ref, qtap_ref, query_raw)
    gate = silu(gate_rows)

    def iota(shape, dim):
        return lax.broadcasted_iota(jnp.int32, shape, dim)

    own_group = lax.div(iota((heads, groups * states), 0), per_group) == lax.div(
        iota((heads, groups * states), 1), states
    )
    own_head = iota((heads, channels), 0) == lax.div(iota((heads, channels), 1), head_dim)
    own_step = iota((heads, LANES), 1) == iota((heads, LANES), 0) + t * heads
    own_rate = iota((heads, heads), 0) == iota((heads, heads), 1)
    rate = jnp.sum(jnp.where(own_rate, rate_ref[...], 0.0), axis=1, keepdims=True)
    rows = []
    for s in range(plan.seqs):
        tail, total, live = prepared[s]
        step_raw = jnp.sum(jnp.where(own_step, step_rows[s : s + 1], 0.0), axis=1, keepdims=True)
        step_size = jnp.maximum(step_raw, 0.0) + jnp.log1p(jnp.exp(-jnp.abs(step_raw)))
        new_decay = -rate * step_size
        query_spread = jnp.where(own_group, new_query[s : s + 1], 0.0)
        key_spread = jnp.where(own_group, new_key[s : s + 1], 0.0)
        scores = lax.dot_general(
            query_spread.astype(jnp.bfloat16),
            keys_ref[s],
            (((1,), (1,)), ((), ())),
            preferred_element_type=jnp.float32,
        )
        weights = jnp.where(live, jnp.exp(tail + new_decay) * steps_ref[s] * scores, 0.0).astype(jnp.bfloat16)
        from_block = jnp.dot(weights, values_ref[s], preferred_element_type=jnp.float32)
        query_heads = query_spread[:, 0:states]
        for g in range(1, groups):
            query_heads = query_heads + query_spread[:, g * states : (g + 1) * states]
        high = query_heads.astype(jnp.bfloat16)
        low = (query_heads - high.astype(jnp.float32)).astype(jnp.bfloat16)

        def contract(rows_in, block):
            return lax.dot_general(
                rows_in, block, (((1,), (1,)), ((), ())), preferred_element_type=jnp.float32
            )

        both = contract(jnp.concatenate([high, low], axis=0), state_high[s])
        from_state = both[0:heads] + both[heads:] + contract(high, state_low[s])
        self_score = jnp.sum(query_spread * key_spread, axis=1, keepdims=True)
        mixed = jnp.exp(total + new_decay) * from_state + from_block
        mixed = mixed + (step_size * self_score) * new_value[s : s + 1]
        mixed = jnp.where(own_head, mixed * gate[s : s + 1], 0.0)
        mean = jnp.sum(mixed * mixed, axis=1, keepdims=True) / head_dim
        mixed = mixed * lax.rsqrt(mean + EPSILON)
        rows.append(jnp.sum(mixed, axis=0, keepdims=True) * head_gain_ref[...])
    return rows


def prepare_block(plan, lengths_ref, decay_ref):
    heads, block_len = decay_ref.shape[1], decay_ref.shape[2]
    after = lax.broadcasted_iota(jnp.int32, (block_len, block_len), 0) > lax.broadcasted_iota(
        jnp.int32, (block_len, block_len), 1
    )
    after = jnp.where(after, 1.0, 0.0)
    position = lax.broadcasted_iota(jnp.int32, (heads, block_len), 1)
    out = []
    for s in range(plan.seqs):
        live = position < lengths_ref[s] - 1
        masked = jnp.where(live, decay_ref[s], 0.0)
        tail = jnp.dot(masked, after, precision=lax.Precision.HIGHEST, preferred_element_type=jnp.float32)
        out.append((tail, jnp.sum(masked, axis=1, keepdims=True), live))
    return out


SMALL = 15
LOADED = 15


def layer_kernel(plan, *refs):
    (x_ref, gain_ref, mix_gain_ref, step_ref, lengths_ref, vtap_ref, ktap_ref, qtap_ref) = refs[:8]
    (vpast_ref, kpast_ref, qpast_ref, rate_ref, head_gain_ref, gain_after_ref, decay_ref) = refs[8:SMALL]
    stored = refs[SMALL : SMALL + LOADED]
    out_ref = refs[SMALL + LOADED]
    rest = refs[SMALL + LOADED + 1 :]
    held, rest = rest[:LOADED], rest[LOADED:]
    load_sem, rest = rest[0], rest[1:]
    (
        gathered,
        gather_sem,
        pair_one,
        pair_sem_one,
        mix_out,
        mix_in,
        mline_out,
        mline_in,
        mplane_sem,
        mline_sem,
        mixed,
        stacked,
        pair_two,
        pair_sem_two,
        final_in,
        final_out,
        section_buf,
        mz_sem,
        mp_sem,
        final_sem,
        state_high,
        state_low,
    ) = rest[:22]
    unit = len(unit_scratch(plan))
    scratch_one, scratch_two = rest[22 : 22 + unit], rest[22 + unit :]
    loads = [pltpu.make_async_copy(stored[n], held[n], load_sem.at[n]) for n in range(LOADED)]
    for load in loads:
        load.start()
    (gate_ref, lift_ref, drop_ref, value_ref, mgate_ref, key_ref, query_ref) = held[:7]
    (keys_ref, values_ref, steps_ref, state_ref, out_proj_ref, gate2_ref, lift2_ref, drop2_ref) = held[7:]

    z, p, t = place(plan)
    inner, outer, group, seqs = plan.inner, plan.outer, plan.group, plan.seqs
    greet(plan, z, p, t)
    first_copy = remote(x_ref, gathered.at[t], gather_sem, (0,), (z * inner + p, 1 - t))
    first_copy.start()
    gathered[t] = x_ref[...]
    prepared = prepare_block(plan, lengths_ref, decay_ref)
    for load in loads[:3]:
        load.wait()
    remote(x_ref, gathered.at[1 - t], gather_sem, (0,), (z * inner + p, 1 - t)).wait_recv()
    x = gathered[...].reshape(plan.rows, plan.width)
    product, sends = unit_product(plan, x, gain_ref[...], gate_ref, lift_ref, drop_ref, scratch_one)
    sends.append(first_copy)
    unit_sum = swap_whole(plan, product, pair_one, pair_sem_one)
    section = (x.astype(jnp.float32) + 0.5 * unit_sum).astype(jnp.bfloat16)
    at = lax.broadcasted_iota(jnp.int32, (plan.rows, plan.rows), 0)
    of = lax.broadcasted_iota(jnp.int32, (plan.rows, plan.rows), 1)
    own_inner = lax.div(at, outer * seqs)
    left = at - own_inner * (outer * seqs)
    own_outer = lax.div(left, seqs)
    wanted = (own_outer * inner + own_inner) * seqs + (left - own_outer * seqs)
    moving = jnp.where(of == wanted, 1.0, 0.0).astype(jnp.bfloat16)
    values = jnp.dot(moving, section, preferred_element_type=jnp.float32)
    squares = jnp.sum(values * values, axis=1, keepdims=True)
    scaled = (values * mix_gain_ref[...]).astype(jnp.bfloat16)
    steps = step_ref.shape[0]
    row = lax.broadcasted_iota(jnp.int32, (LANES, steps), 0)
    lane = lax.broadcasted_iota(jnp.int32, (LANES, steps), 1)
    spread = jnp.where(row == lane, 1.0, 0.0).astype(jnp.bfloat16)
    step_wide = jnp.dot(spread, step_ref[...], preferred_element_type=jnp.float32).astype(jnp.bfloat16)
    lanes = lax.broadcasted_iota(jnp.int32, (plan.rows, LANES), 1)
    last = lax.dot_general(scaled, step_wide, (((1,), (1,)), ((), ())), preferred_element_type=jnp.float32)
    last = jnp.where(lanes == LANES - 1, squares, last).astype(jnp.bfloat16)
    for load in loads[3:7]:
        load.wait()
    chunks, first = [], 0
    plane = []
    for n, parts in enumerate(((key_ref, query_ref), (value_ref,), (mgate_ref,))):
        low = first
        pieces = [jnp.dot(scaled, ref[...], preferred_element_type=jnp.float32).astype(jnp.bfloat16) for ref in parts]
        if n == 0:
            pieces.append(last)
        for piece in pieces:
            size = piece.shape[1]
            for q in range(inner):
                mix_out[q, :, first : first + size] = piece[q * group : (q + 1) * group]
            first = first + size
        columns = slice(low, first)
        chunks.append(columns)
        copies = []
        for d in range(1, inner):
            copy = remote(
                mix_out.at[lax.rem(p + d, inner), :, columns],
                mix_in.at[d, :, columns],
                mplane_sem,
                (d, n),
                plane_peer(plan, z, p, t, d),
            )
            copy.start()
            copies.append(copy)
        plane.append(copies)
        sends.extend(copies)
    for load in loads[7:]:
        load.wait()
    for s in range(seqs):
        state = state_ref[s]
        high = state.astype(jnp.bfloat16)
        state_high[s] = high
        state_low[s] = (state - high.astype(jnp.float32)).astype(jnp.bfloat16)
    line = []
    for n, columns in enumerate(chunks):
        total = mix_out[p, :, columns].astype(jnp.float32)
        for d in range(1, inner):
            plane[n][d - 1].wait_recv()
            total = total + mix_in[d, :, columns].astype(jnp.float32)
        for o in range(outer):
            mline_out[o, :, columns] = total[o * seqs : (o + 1) * seqs].astype(mline_out.dtype)
        copies = []
        for d in range(1, outer):
            copy = remote(
                mline_out.at[lax.rem(z + d, outer), :, columns],
                mline_in.at[d, :, columns],
                mline_sem,
                (d, n),
                line_peer(plan, z, p, t, d),
            )
            copy.start()
            copies.append(copy)
        line.append(copies)
        sends.extend(copies)
    totals = []
    for n, columns in enumerate(chunks):
        total = mline_out[z, :, columns].astype(jnp.float32)
        for d in range(1, outer):
            line[n][d - 1].wait_recv()
            total = total + mline_in[d, :, columns].astype(jnp.float32)
        totals.append(total)
    scale = lax.rsqrt(totals[0][:, -1:] / plan.model + EPSILON)
    totals = [total * scale for total in totals]
    keys_end, query_end = key_ref.shape[1], key_ref.shape[1] + query_ref.shape[1]
    raw = (
        totals[0][:, :keys_end],
        totals[0][:, keys_end:query_end],
        totals[0][:, query_end:],
        totals[1],
        totals[2],
    )
    rows = block_mix(
        plan,
        raw,
        lengths_ref,
        vtap_ref,
        ktap_ref,
        qtap_ref,
        vpast_ref,
        kpast_ref,
        qpast_ref,
        rate_ref,
        head_gain_ref,
        state_high,
        state_low,
        keys_ref,
        values_ref,
        steps_ref,
        decay_ref,
        prepared,
    )
    mixed[z, p] = jnp.concatenate(rows, axis=0).astype(mixed.dtype)
    own = mixed.at[z, p]
    for d in range(1, outer):
        copy = remote(own, own, mz_sem, (d,), line_peer(plan, z, p, t, d))
        copy.start()
        sends.append(copy)
    for n in range(outer):
        source = lax.rem(z + outer - n, outer)
        block = mixed.at[source, p]
        if n > 0:
            remote(block, block, mz_sem, (n,), line_peer(plan, z, p, t, n)).wait_recv()
        for d in range(1, inner):
            copy = remote(block, block, mp_sem, (d, n), plane_peer(plan, z, p, t, d))
            copy.start()
            sends.append(copy)
    for n in range(outer):
        source = lax.rem(z + outer - n, outer)
        for d in range(1, inner):
            block = mixed.at[source, lax.rem(p + inner - d, inner)]
            remote(block, block, mp_sem, (d, n), plane_peer(plan, z, p, t, d)).wait_recv()
    for o in range(outer):
        for i in range(inner):
            first = (o * inner + i) * seqs
            stacked[first : first + seqs, :] = mixed[o, i].astype(jnp.float32)
    product = jnp.dot(
        stacked[...].astype(jnp.bfloat16), out_proj_ref[...], preferred_element_type=jnp.float32
    ).astype(jnp.bfloat16)
    branch = swap_whole(plan, product, pair_two, pair_sem_two)
    x = (section.astype(jnp.float32) + branch).astype(jnp.bfloat16)
    section_buf[...] = x.reshape(section_buf.shape)
    product, more = unit_product(plan, x, gain_after_ref[...], gate2_ref, lift2_ref, drop2_ref, scratch_two)
    final_out[...] = product.reshape(final_out.shape)
    copy = remote(final_out.at[1 - t], final_in, final_sem, (0,), (z * inner + p, 1 - t))
    copy.start()
    copy.wait()
    unit_sum = final_out[t].astype(jnp.float32) + final_in[...].astype(jnp.float32)
    out_ref[...] = (section_buf[t].astype(jnp.float32) + 0.5 * unit_sum).astype(jnp.bfloat16)
    for copy in sends + more:
        copy.wait_send()


def on_device_fast(
    hidden_in,
    gain_before,
    gate_before,
    lift_before,
    drop_before,
    mixer_gain,
    value_proj,
    gate_proj,
    key_proj,
    query_proj,
    step_proj,
    value_taps,
    key_taps,
    query_taps,
    value_past,
    key_past,
    query_past,
    decay_rate,
    block_state,
    block_keys,
    block_values,
    block_steps,
    block_decay,
    lengths,
    head_gain,
    out_proj,
    gain_after,
    gate_after,
    lift_after,
    drop_after,
):
    kv, tp = lax.axis_size("kv"), lax.axis_size("tp")
    own_rows, width = hidden_in.shape
    rows, hidden, seqs = own_rows * tp, gate_before.shape[1], lengths.shape[0]
    plan = Plan(kv, rows, own_rows, width, hidden, seqs)
    channels = value_proj.shape[1]
    span = channels + gate_proj.shape[1] + key_proj.shape[1] + query_proj.shape[1] + LANES
    i, o, g, s = plan.inner, plan.outer, plan.group, seqs
    vmem = pl.BlockSpec(memory_space=pltpu.VMEM)
    smem = pl.BlockSpec(memory_space=pltpu.SMEM)
    anywhere = pl.BlockSpec(memory_space=pl.ANY)
    small = (
        hidden_in,
        gain_before[None],
        mixer_gain[None],
        step_proj.T,
        lengths,
        value_taps,
        key_taps,
        query_taps,
        value_past.transpose(1, 0, 2),
        key_past.transpose(1, 0, 2),
        query_past.transpose(1, 0, 2),
        decay_rate[None],
        head_gain[None],
        gain_after[None],
        block_decay.transpose(0, 2, 1),
    )
    loaded = (
        gate_before,
        lift_before,
        drop_before,
        value_proj,
        gate_proj,
        key_proj,
        query_proj,
        block_keys,
        block_values,
        block_steps.transpose(0, 2, 1),
        block_state.reshape(seqs, channels, block_state.shape[3]),
        out_proj,
        gate_after,
        lift_after,
        drop_after,
    )
    dma, half, full = pltpu.SemaphoreType.DMA, jnp.bfloat16, jnp.float32
    scratch = [pltpu.VMEM(array.shape, array.dtype) for array in loaded] + [
        dma((len(loaded),)),
        pltpu.VMEM((2, own_rows, width), half),
        dma((2, 1)),
        pltpu.VMEM((2, rows, width), half),
        dma((2, 1)),
        pltpu.VMEM((i, g, span), half),
        pltpu.VMEM((i, g, span), half),
        pltpu.VMEM((o, s, span), SHORT),
        pltpu.VMEM((o, s, span), SHORT),
        dma((2, i, 3)),
        dma((2, o, 3)),
        pltpu.VMEM((o, i, s, channels), SHORT),
        pltpu.VMEM((rows, channels), full),
        pltpu.VMEM((2, rows, width), half),
        dma((2, 1)),
        pltpu.VMEM((own_rows, width), half),
        pltpu.VMEM((2, own_rows, width), half),
        pltpu.VMEM((2, own_rows, width), half),
        dma((2, o)),
        dma((2, i, o)),
        dma((2, 1)),
        pltpu.VMEM((s, channels, block_state.shape[3]), half),
        pltpu.VMEM((s, channels, block_state.shape[3]), half),
    ]
    return pl.pallas_call(
        functools.partial(layer_kernel, plan),
        out_shape=jax.ShapeDtypeStruct((own_rows, width), jnp.bfloat16),
        in_specs=[smem if array is lengths else vmem for array in small] + [anywhere] * len(loaded),
        out_specs=vmem,
        scratch_shapes=scratch + unit_scratch(plan) + unit_scratch(plan),
        compiler_params=pltpu.CompilerParams(collective_id=0, has_side_effects=True),
        name="layer",
    )(*small, *loaded)


def gather_rows(rows_in, gain_vec):
    whole_rows = lax.all_gather(rows_in, "tp", axis=0, tiled=True)
    values = whole_rows.astype(jnp.float32)
    squares = jnp.sum(values * values, axis=1)
    scaled = (values * gain_vec[None, :]).astype(jnp.bfloat16)
    return (scaled, squares)


def inverse_scale(totals):
    return lax.rsqrt(totals / D + EPSILON)[:, None]


def own_rows(totals, row_count):
    return lax.dynamic_slice_in_dim(totals, lax.axis_index("kv") * row_count, row_count, 0)


def finish(partial_value):
    return lax.psum_scatter(
        partial_value.astype(jnp.float32).astype(jnp.bfloat16),
        "tp",
        scatter_dimension=0,
        tiled=True,
    ).astype(jnp.float32)


def half_mlp(rows_in, gain_vec, gate_weight, lift_weight, drop_weight):
    scaled, squares = gather_rows(rows_in, gain_vec)
    totals = lax.psum(squares, "kv")
    gate_part = jnp.dot(scaled, gate_weight, preferred_element_type=jnp.float32)
    lift_part = jnp.dot(scaled, lift_weight, preferred_element_type=jnp.float32)
    gate_sum, lift_sum = lax.psum((gate_part, lift_part), "kv")
    row_scale = inverse_scale(totals)
    hidden = (jax.nn.silu(gate_sum * row_scale) * (lift_sum * row_scale)).astype(jnp.bfloat16)
    partial_value = jnp.dot(hidden, drop_weight, preferred_element_type=jnp.float32).astype(
        jnp.bfloat16
    )
    return finish(partial_value)


def convolve(past_rows, taps, newest):
    earlier = jnp.sum(past_rows.astype(jnp.float32) * taps[None, :-1, :], axis=1)
    return jax.nn.silu(earlier + taps[-1][None, :] * newest)


def mixer(
    rows_in,
    mixer_gain,
    value_proj,
    gate_proj,
    key_proj,
    query_proj,
    step_proj,
    value_taps,
    key_taps,
    query_taps,
    value_past,
    key_past,
    query_past,
    decay_rate,
    block_state,
    block_keys,
    block_values,
    block_steps,
    block_decay,
    lengths,
    head_gain,
    out_proj,
):
    scaled, squares = gather_rows(rows_in, mixer_gain)
    seq_count = lengths.shape[0]
    value_part = jnp.dot(scaled, value_proj, preferred_element_type=jnp.float32)
    gate_part = jnp.dot(scaled, gate_proj, preferred_element_type=jnp.float32)
    key_part = jnp.dot(scaled, key_proj, preferred_element_type=jnp.float32)
    query_part = jnp.dot(scaled, query_proj, preferred_element_type=jnp.float32)
    step_part = jnp.dot(scaled, step_proj, preferred_element_type=jnp.float32)
    totals = own_rows(lax.psum(squares, "kv"), seq_count)
    value_raw, gate_raw, key_raw, query_raw, step_all = (
        lax.psum_scatter(value_part, "kv", scatter_dimension=0, tiled=True),
        lax.psum_scatter(gate_part, "kv", scatter_dimension=0, tiled=True),
        lax.psum_scatter(key_part, "kv", scatter_dimension=0, tiled=True),
        lax.psum_scatter(query_part, "kv", scatter_dimension=0, tiled=True),
        lax.psum_scatter(step_part, "kv", scatter_dimension=0, tiled=True),
    )
    row_scale = inverse_scale(totals)
    heads_here = decay_rate.shape[0]
    step_raw = (
        lax.dynamic_slice_in_dim(step_all, lax.axis_index("tp") * heads_here, heads_here, 1)
        * row_scale
    )
    new_value = convolve(value_past, value_taps, value_raw * row_scale)
    gate_vals = gate_raw * row_scale
    new_key = convolve(key_past, key_taps, key_raw * row_scale)
    new_query = convolve(query_past, query_taps, query_raw * row_scale)
    step_size = jax.nn.softplus(step_raw)
    new_decay = -decay_rate[None, :] * step_size
    block_len = block_keys.shape[1]
    head_dim = block_state.shape[2]
    state_size = block_state.shape[3]
    per_group = HEADS // GROUPS
    group_count = heads_here // per_group
    live_mask = (jnp.arange(block_len, dtype=jnp.int32)[None, :] < (lengths - 1)[:, None])[
        :, :, None
    ]
    masked = jnp.where(live_mask, block_decay, 0.0)
    running = jnp.cumsum(masked, axis=1)
    block_total = running[:, -1, :]
    tail_sum = block_total[:, None, :] - running
    query_round = new_query.astype(jnp.bfloat16).reshape(seq_count, group_count, state_size)
    scores = jnp.einsum(
        "slgn,sgn->slg",
        block_keys.reshape(seq_count, block_len, group_count, state_size),
        query_round,
        preferred_element_type=jnp.float32,
    )
    scores = jnp.repeat(scores, per_group, axis=2)
    weights = jnp.where(
        live_mask, jnp.exp(tail_sum + new_decay[:, None, :]) * block_steps * scores, 0.0
    ).astype(jnp.bfloat16)
    from_block = jnp.einsum(
        "slh,slhp->shp",
        weights,
        block_values.reshape(seq_count, block_len, heads_here, head_dim),
        preferred_element_type=jnp.float32,
    )
    query_heads = jnp.repeat(
        new_query.reshape(seq_count, group_count, state_size), per_group, axis=1
    )
    source_state = jnp.einsum(
        "shpn,shn->shp", block_state, query_heads, precision=lax.Precision.HIGHEST
    )
    source_state = source_state * jnp.exp(block_total + new_decay)[:, :, None]
    self_score = jnp.repeat(
        jnp.sum((new_query * new_key).reshape(seq_count, group_count, state_size), axis=2),
        per_group,
        axis=1,
    )
    from_token = (step_size * self_score)[:, :, None] * new_value.reshape(
        seq_count, heads_here, head_dim
    )
    gated_out = (source_state + from_block + from_token) * jax.nn.silu(
        gate_vals.reshape(seq_count, heads_here, head_dim)
    )
    normed = gated_out * lax.rsqrt(jnp.mean(gated_out * gated_out, axis=2, keepdims=True) + EPSILON)
    normed = normed * head_gain.reshape(heads_here, head_dim)[None]
    mixed_rows = normed.reshape(seq_count, heads_here * head_dim).astype(jnp.bfloat16)
    partial_value = jnp.dot(
        lax.all_gather(mixed_rows, "kv", axis=0, tiled=True),
        out_proj,
        preferred_element_type=jnp.float32,
    ).astype(jnp.bfloat16)
    return finish(partial_value)


def on_device(
    hidden_in,
    gain_before,
    gate_before,
    lift_before,
    drop_before,
    mixer_gain,
    value_proj,
    gate_proj,
    key_proj,
    query_proj,
    step_proj,
    value_taps,
    key_taps,
    query_taps,
    value_past,
    key_past,
    query_past,
    decay_rate,
    block_state,
    block_keys,
    block_values,
    block_steps,
    block_decay,
    lengths,
    head_gain,
    out_proj,
    gain_after,
    gate_after,
    lift_after,
    drop_after,
):
    section_one = (
        hidden_in.astype(jnp.float32)
        + 0.5 * half_mlp(hidden_in, gain_before, gate_before, lift_before, drop_before)
    ).astype(jnp.bfloat16)
    branch_mix = mixer(
        section_one,
        mixer_gain,
        value_proj,
        gate_proj,
        key_proj,
        query_proj,
        step_proj,
        value_taps,
        key_taps,
        query_taps,
        value_past,
        key_past,
        query_past,
        decay_rate,
        block_state,
        block_keys,
        block_values,
        block_steps,
        block_decay,
        lengths,
        head_gain,
        out_proj,
    )
    section_two = (section_one.astype(jnp.float32) + branch_mix).astype(jnp.bfloat16)
    return (
        section_two.astype(jnp.float32)
        + 0.5 * half_mlp(section_two, gain_after, gate_after, lift_after, drop_after)
    ).astype(jnp.bfloat16)


def fits(
    hidden_in,
    gain_before,
    gate_before,
    lift_before,
    drop_before,
    mixer_gain,
    value_proj,
    gate_proj,
    key_proj,
    query_proj,
    step_proj,
    value_taps,
    key_taps,
    query_taps,
    value_past,
    key_past,
    query_past,
    decay_rate,
    block_state,
    block_keys,
    block_values,
    block_steps,
    block_decay,
    lengths,
    head_gain,
    out_proj,
    gain_after,
    gate_after,
    lift_after,
    drop_after,
):
    kv, tp = lax.axis_size("kv"), lax.axis_size("tp")
    own_rows, width = hidden_in.shape
    inner = max(i for i in range(1, math.isqrt(kv) + 1) if kv % i == 0)
    aligned = (
        gate_before.shape[1],
        width,
        value_proj.shape[1],
        gate_proj.shape[1],
        key_proj.shape[1],
        query_proj.shape[1],
    )
    return (
        tp == 2
        and inner > 1
        and all(size % LANES == 0 for size in aligned)
        and own_rows % 16 == 0
        and own_rows * tp % (16 * inner) == 0
        and lengths.shape[0] in (4, 8)
        and lengths.shape[0] * kv == own_rows * tp
        and step_proj.shape[1] < LANES
        and gate_before.shape[1] // LANES >= 2 * (kv // inner)
    )


def choose(*args):
    return on_device_fast(*args) if fits(*args) else on_device(*args)


def solution(mesh):
    return jax.shard_map(
        choose,
        mesh=mesh,
        in_specs=(
            P("tp", "kv"),
            P("kv"),
            P("kv", "tp"),
            P("kv", "tp"),
            P("tp", "kv"),
            P("kv"),
            P("kv", "tp"),
            P("kv", "tp"),
            P("kv", "tp"),
            P("kv", "tp"),
            P("kv", None),
            P(None, "tp"),
            P(None, "tp"),
            P(None, "tp"),
            P("kv", None, "tp"),
            P("kv", None, "tp"),
            P("kv", None, "tp"),
            P("tp"),
            P("kv", "tp", None, None),
            P("kv", None, "tp"),
            P("kv", None, "tp"),
            P("kv", None, "tp"),
            P("kv", None, "tp"),
            P("kv"),
            P("tp"),
            P("tp", "kv"),
            P("kv"),
            P("kv", "tp"),
            P("kv", "tp"),
            P("tp", "kv"),
        ),
        out_specs=P("tp", "kv"),
        check_vma=False,
    )
```
